256 devices in a mesh: kv: 64 (over z, y, core), tp: 4 (over x).
Axes of the slice: x: 4, y: 4, z: 8, core: 2. Of those that a mesh axis runs over, the one named last changes fastest.
Arguments:
- tokens: bfloat16 [24576, 1024], P('kv', 'tp'), may hold values from -6 to 6
- query_weight: bfloat16 [1024, 512], P(None, 'tp'), may hold values from -0.1875 to 0.1875
- key_weight: bfloat16 [1024, 512], P(None, 'tp'), may hold values from -0.1875 to 0.1875
- value_weight: bfloat16 [1024, 512], P(None, 'tp'), may hold values from -0.1875 to 0.1875
- out_weight: bfloat16 [512, 1024], P('tp'), may hold values from -0.25 to 0.25
- norm_gain: float32 [512], P('tp'), may hold values from 0.1 to 1.9
- chosen_owner: int32 [384, 8], P('kv'), may hold values from 0 to 63, all different within a row; in each aligned block of 6 rows (0 to 5, 6 to 11, ...) at most 1 rows name the same one
- chosen_local: int32 [384, 8], P('kv'), may hold values from 0 to 5
Outputs:
- attended_out: bfloat16 [24576, 1024], P('kv', 'tp')
The draws below stay inside these ranges and needn't reach their ends.
Inputs may be any that keep to these rules, and one draw needn't show every extreme that they name: `chosen_owner`: each row names 8 different owners; among the 6 rows of one device no owner is named by more than 1 rows, and in some device's rows one owner is named by exactly 1. `chosen_local`: any index of a key block within its owner.
All inputs are finite; a program needn't handle non-finite values.
Results may differ from the reference program's by a relative error of at most 0.015.
Values may be sent and summed in bfloat16 or wider, within the bound.
A program may use at most 64 MiB of HBM per device.

```python
import math
import jax
import jax.numpy as jnp
import numpy as np
from jax import lax

WIDTH = 1024
HEADS = 8
HEAD_SIZE = 64
BLOCK = 64
CHOSEN = 8
QB_DEV = 6
TOKENS = 24576
BLOCKS_ALL = 384
CAP = 1
N_KV = 64


def with_ends(drawn, key, least, high):
    shape = drawn.shape
    spot = [jax.random.randint(jax.random.fold_in(key, axis), (), 0, shape[axis]) for axis in range(len(shape))]
    drawn = drawn.at[tuple(spot)].set(least)
    longest = shape.index(max(shape))
    spot[longest] = (spot[longest] + 1) % shape[longest]
    return drawn.at[tuple(spot)].set(high)


def level_of(own_key, dims, split, least, largest):
    loudness = 1.0
    for axis_at, shards_of in split:
        draws = jax.random.uniform(jax.random.fold_in(jax.random.fold_in(own_key, 6), axis_at), (shards_of,), jnp.float32, least / len(split), largest / len(split))
        loudness = loudness * jnp.repeat(jnp.exp(draws), dims[axis_at] // shards_of).reshape((-1,) + (1,) * (len(dims) - 1 - axis_at))
    return loudness


def deal_out(key, own, number, rows, amount, top, most, lean):
    sequence = jax.random.permutation(key, amount)
    heavy_load, usual = shares(amount, rows * top, most, lean, True), shares(amount, rows * top, most, lean, False)
    places = jnp.arange(amount)

    def named(sizes, turn):
        used = int((sizes > 0).sum())
        fixed = max(1, used // 4)
        shifted = fixed + (places - fixed + turn * (used - fixed)) % max(1, amount - fixed)
        return jnp.zeros((amount,), jnp.int32).at[sequence[jnp.where(places < fixed, places, shifted)]].set(jnp.asarray(sizes, jnp.int32))

    sizes = jnp.where(number % 4 == 0, named(heavy_load, number // 4), named(usual, number - number // 4 - 1))
    mixed = jax.random.permutation(jax.random.fold_in(own, 3), amount)
    giver, receiver = mixed[0:amount // 2 * 2:2], mixed[1:amount // 2 * 2:2]
    margin = jnp.minimum(sizes[giver] - 1, most - sizes[receiver]) // 2
    margin = jnp.where((giver == sequence[0]) | (receiver == sequence[0]) | (sizes[receiver] == 0), 0, jnp.maximum(margin, 0))
    shifted = jax.random.randint(jax.random.fold_in(own, 4), (amount // 2,), 0, 1 << 20) % (margin + 1)
    sizes = sizes.at[giver].add(-shifted).at[receiver].add(shifted)
    items = jnp.searchsorted(jnp.cumsum(sizes), jnp.arange(rows * top), side="right").astype(jnp.int32)
    listing = items.reshape(top, rows).T
    listing = listing[jax.random.permutation(jax.random.fold_in(own, 1), rows)]
    turn = jax.random.randint(jax.random.fold_in(own, 2), (rows, 1), 0, top)
    return jnp.take_along_axis(listing, (jnp.arange(top)[None, :] + turn) % top, axis=1)


def shares(amount, total, reach, lean, full):
    weights = [(1 << 20) // math.isqrt(grade ** lean) + 1 for grade in range(1, amount + 1)]
    largest = reach if full else min(reach, max(-(-total // amount), total * weights[0] // sum(weights)))
    least = 1 if total - largest >= amount - 1 else 0
    counts, rest = [largest] + [least] * (amount - 1), total - largest - least * (amount - 1)
    while rest > 0:
        candidates = [i for i in range(1, amount) if counts[i] < largest] or [i for i in range(1, amount) if counts[i] < reach]
        mass, left = sum([weights[i] for i in candidates]), rest
        for i in candidates:
            more = min(reach - counts[i], max(1, left * weights[i] // mass), rest)
            counts[i] = counts[i] + more
            rest = rest - more
    return np.array(counts)


def noise(key, shape, scale, limit, shards=(), kind=jnp.bfloat16):
    array = scale * jax.random.normal(key, shape, jnp.float32)
    if shards:
        array = array * level_of(key, shape, shards, -0.22, 0.18)
    return jnp.clip(array, -limit, limit).astype(kind)


def setup_inputs(seed: int = 0) -> dict:
    keys = jax.random.split(jax.random.key(seed), 9)
    tokens = noise(keys[0], (TOKENS, WIDTH), 1.0, 6.0, ((0, 64), (1, 4)))
    query_weight = noise(keys[1], (WIDTH, HEADS * HEAD_SIZE), WIDTH ** -0.5, 0.1875, ((1, 4),))
    key_weight = noise(keys[2], (WIDTH, HEADS * HEAD_SIZE), WIDTH ** -0.5, 0.1875, ((1, 4),))
    value_weight = noise(keys[3], (WIDTH, HEADS * HEAD_SIZE), WIDTH ** -0.5, 0.1875, ((1, 4),))
    out_weight = noise(keys[4], (HEADS * HEAD_SIZE, WIDTH), (HEADS * HEAD_SIZE) ** -0.5, 0.25, ((0, 4),))
    norm_gain = jnp.clip(1.0 + 0.18 * jax.random.normal(keys[5], (HEADS * HEAD_SIZE,), jnp.float32), 0.1, 1.9)
    chosen_owner_keys = jax.random.split(jax.random.fold_in(keys[6], 1), BLOCKS_ALL // QB_DEV)
    chosen_owner_turns = jax.random.permutation(jax.random.fold_in(keys[6], 3), BLOCKS_ALL // QB_DEV)
    chosen_owner = jax.vmap(lambda own, number: deal_out(jax.random.fold_in(keys[6], 2), own, number, QB_DEV, N_KV, CHOSEN, CAP, 2))(chosen_owner_keys, chosen_owner_turns).reshape((BLOCKS_ALL, CHOSEN))
    chosen_local = with_ends(jax.random.randint(keys[7], (BLOCKS_ALL, CHOSEN), 0, QB_DEV), jax.random.fold_in(keys[7], 1), 0, QB_DEV - 1).astype(jnp.int32)
    return dict(tokens=tokens, query_weight=query_weight, key_weight=key_weight, value_weight=value_weight, out_weight=out_weight, norm_gain=norm_gain, chosen_owner=chosen_owner, chosen_local=chosen_local)


neg_fill = -1e+30
eps_norm = 1e-06

def project(tokens, weight):
    return jnp.dot(tokens, weight, preferred_element_type=jnp.float32).astype(jnp.bfloat16)

def reference(tokens, query_weight, key_weight, value_weight, out_weight, norm_gain, chosen_owner, chosen_local):
    block_count = QB_DEV * N_KV
    queries = project(tokens, query_weight).reshape(block_count, BLOCK, HEADS, HEAD_SIZE)
    keys_all = project(tokens, key_weight).reshape(block_count, BLOCK, HEADS, HEAD_SIZE)
    values_all = project(tokens, value_weight).reshape(block_count, BLOCK, HEADS, HEAD_SIZE)
    picked = (chosen_owner * QB_DEV + chosen_local).astype(jnp.int32)
    listed_all = jnp.concatenate([jnp.arange(block_count, dtype=jnp.int32)[:, None], picked], axis=1)
    offsets = jnp.arange(BLOCK, dtype=jnp.int32)
    score_scale = HEAD_SIZE ** (-0.5)
    entry_first = (jnp.arange(CHOSEN + 1, dtype=jnp.int32) == 0)[:, None]

    def attend(packed):
        block_index, listed = packed
        query_rows = queries[block_index].astype(jnp.float32)
        key_rows = keys_all[listed].astype(jnp.float32)
        value_rows = values_all[listed].astype(jnp.float32)
        scores = jnp.einsum('qhd,cthd->hqct', query_rows, key_rows, precision=lax.Precision.HIGHEST) * score_scale
        query_pos = block_index * BLOCK + offsets
        key_pos = jnp.where(entry_first, listed[:, None] * BLOCK + offsets[None, :], jnp.int32(-1))
        visible = key_pos[None, :, :] <= query_pos[:, None, None]
        scores = jnp.where(visible[None], scores, neg_fill)
        highest = lax.optimization_barrier(jnp.max(scores, axis=(2, 3), keepdims=True))
        weights = jnp.where(visible[None], jnp.exp(scores - highest), jnp.float32(0.0))
        mass_sum = lax.optimization_barrier(jnp.sum(weights, axis=(2, 3)))
        blended = jnp.einsum('hqct,cthd->qhd', weights, value_rows, precision=lax.Precision.HIGHEST)
        return (blended / mass_sum.T[:, :, None]).astype(jnp.bfloat16)
    attended = lax.map(attend, (jnp.arange(block_count, dtype=jnp.int32), listed_all))
    attended = attended.reshape(block_count * BLOCK, HEADS * HEAD_SIZE)
    wide_rows = attended.astype(jnp.float32)
    mean_sq = lax.optimization_barrier(jnp.mean(wide_rows * wide_rows, axis=1, keepdims=True))
    normed = (wide_rows * lax.rsqrt(mean_sq + eps_norm) * norm_gain.astype(jnp.float32)).astype(jnp.bfloat16)
    return jnp.dot(normed, out_weight, preferred_element_type=jnp.float32).astype(jnp.bfloat16)
```

```python
import jax
import jax.numpy as jnp
from jax import lax
from jax.experimental import pallas as pl
from jax.experimental.pallas import tpu as pltpu
from jax.sharding import PartitionSpec as P

MESH = pl.DeviceIdType.MESH
BF16, F32, I32 = jnp.bfloat16, jnp.float32, jnp.int32

HEADS = 8
HEAD_SIZE = 64
BLOCK = 64
CHOSEN = 8
NB = 6
FEATS = 128
PART = 256
NZ, NY, NX = 8, 4, 4
NEG = -1e30
EPS = 1e-06
CH = 3
VMEM, SMEM, DMA = pltpu.VMEM, pltpu.SMEM, pltpu.SemaphoreType.DMA

NT = (((1,), (1,)), ((), ()))
NN = (((1,), (0,)), ((), ()))


def dot(a, b, dims=NN):
    return lax.dot_general(a, b, dims, preferred_element_type=F32)


def sems(**shapes):
    found = {}
    for name, shape in shapes.items():
        found["s_" + name] = DMA(shape)
        found["r_" + name] = DMA(shape)
    return found


def place():
    kv, x = lax.axis_index("kv"), lax.axis_index("tp")
    return lax.rem(kv, 2), lax.rem(lax.div(kv, 2), NY), lax.div(kv, 2 * NY), x


def device(dz=0, dy=0, dx=0, flip=False):
    c, y, z, x = place()
    zz, yy, xx = lax.rem(z + dz, NZ), lax.rem(y + dy, NY), lax.rem(x + dx, NX)
    return ((zz * NY + yy) * 2 + (1 - c if flip else c), xx)


def sender(r):
    def send(src, dst, name, index, to):
        return pltpu.make_async_remote_copy(
            src_ref=src,
            dst_ref=dst,
            send_sem=r["s_" + name].at[index],
            recv_sem=r["r_" + name].at[index],
            device_id=to,
            device_id_type=MESH,
        )

    return send


def greet(peers):
    barrier = pltpu.get_barrier_semaphore()
    for peer in peers:
        pl.semaphore_signal(barrier, inc=1, device_id=peer, device_id_type=MESH)
    return lambda: pl.semaphore_wait(barrier, len(peers))


def rows_of(i, n=BLOCK):
    return pl.ds(i * n, n)


def masks():
    lane = lax.broadcasted_iota(I32, (BLOCK, FEATS), 1)
    sub = lax.broadcasted_iota(I32, (BLOCK, FEATS), 0)
    low = (lane < HEAD_SIZE).astype(F32).astype(BF16)
    high = (lane >= HEAD_SIZE).astype(F32).astype(BF16)
    pick = (lax.rem(lane, HEAD_SIZE) == sub).astype(F32).astype(BF16)
    visible = sub <= lax.rem(lane, HEAD_SIZE)

    def spread(a):
        return jnp.concatenate([a * low, a * high], axis=0)

    return spread, pick, visible


def project_scratch():
    shapes = {f"tok{j}": VMEM((NB * BLOCK, PART), BF16) for j in range(4)}
    shapes["w"] = VMEM((1024, 3 * FEATS), BF16)
    shapes["s_in"] = DMA((4,))
    return shapes | sems(x=(3, NB))


def project(tok_hbm, wq_hbm, wk_hbm, wv_hbm, kv_ref, q_ref, *refs):
    r = dict(zip(project_scratch(), refs))
    x = lax.axis_index("tp")
    send = sender(r)
    ins = [pltpu.make_async_copy(tok_hbm, r["tok0"], r["s_in"].at[0])]
    for n, ref in enumerate((wk_hbm, wv_hbm, wq_hbm)):
        ins.append(pltpu.make_async_copy(ref, r["w"].at[:, pl.ds(n * FEATS, FEATS)], r["s_in"].at[n + 1]))
    for copy in ins:
        copy.start()
    greeted = greet([device(dx=j) for j in (1, 2, 3)])
    spread, pick, _ = masks()
    ins[0].wait()
    greeted()

    def x_own(kind, i):
        dst, dx = ("tok1", 1) if kind == 0 else ("tok3", 3)
        return send(r["tok0"].at[rows_of(i)], r[dst].at[rows_of(i)], "x", (kind, i), device(dx=dx))

    def x_far(i):
        src, dx = ("tok1", 1) if i % 2 == 0 else ("tok3", 3)
        return send(r[src].at[rows_of(i)], r["tok2"].at[rows_of(i)], "x", (2, i), device(dx=dx))

    for i in (0, 1):
        x_own(0, i).start()
        x_own(1, i).start()
    for copy in ins[1:]:
        copy.wait()

    def block(i):
        x_far(i).wait_recv()
        total = jnp.zeros((BLOCK, 3 * FEATS), F32)
        for j in range(4):
            part = pl.ds(pl.multiple_of(lax.rem(x + NX - j, NX) * PART, PART), PART)
            total = total + dot(r[f"tok{j}"][rows_of(i), :], r["w"][part, :])
        kv_ref[i, 0] = total[:, :FEATS].astype(BF16)
        kv_ref[i, 1] = dot(pick, spread(total[:, FEATS : 2 * FEATS].astype(BF16)), NT).astype(BF16)
        q_ref[i] = total[:, 2 * FEATS :].astype(BF16)

    for i in range(NB):
        x_own(0, i).wait_recv()
        x_own(1, i).wait_recv()
        x_far(i).start()
        if i + 2 < NB:
            x_own(0, i + 2).start()
            x_own(1, i + 2).start()
        if i >= 1:
            block(i - 1)
    block(NB - 1)
    for i in range(NB):
        x_own(0, i).wait_send()
        x_own(1, i).wait_send()
        x_far(i).wait_send()


def attend_scratch():
    shapes = {}
    for j in range(4):
        shapes[f"codes{j}"] = VMEM((8, 128), I32)
        if j:
            shapes[f"q{j}"] = VMEM((NB, BLOCK, FEATS), BF16)
    for dz in range(-3, 5):
        if dz:
            shapes[f"kv{dz}"] = VMEM((NB, 2, BLOCK, FEATS), BF16)
        shapes[f"other{dz}"] = VMEM((NB, 2, BLOCK, FEATS), BF16)
    shapes["codes_s"] = SMEM((4, 8, 128), I32)
    for name in ("p", "r"):
        shapes[name + "o"] = VMEM((3, NB, BLOCK, FEATS), BF16)
        shapes[name + "m"] = VMEM((3, NB, 8, FEATS), F32)
    shapes["item_o"] = VMEM((4, 2 * NZ, BLOCK, FEATS), F32)
    shapes["item_m"] = VMEM((4, 2 * NZ, 8, FEATS), F32)
    shapes["own_o"] = VMEM((NB, BLOCK, FEATS), F32)
    shapes["own_m"] = VMEM((NB, 8, FEATS), F32)
    shapes["s_codes"] = DMA((4,))
    return shapes | sems(z=(2, 4, NB), p=(8,), y=(4,), c=(4,), b=(4, CH), m=(4, CH))


def attend_all(kv_ref, q_ref, owner_ref, local_ref, out_ref, *refs):
    r = dict(zip(attend_scratch(), refs))
    r["kv0"], r["q0"] = kv_ref, q_ref
    c, y, z, x = place()
    send = sender(r)
    peers = [device(dy=j) for j in (1, 2, 3)] + [device(dz=1), device(dz=NZ - 1), device(flip=True)]
    greeted = greet(peers)

    lane8 = lax.broadcasted_iota(I32, (8, 128), 1)
    row8 = lax.broadcasted_iota(I32, (8, 128), 0)
    by_owner = jnp.zeros((8, 128), I32)
    listed = jnp.zeros((8, 128), I32)
    for row in range(NB):
        for ch in range(CHOSEN):
            owner = owner_ref[row, ch]
            by_owner = jnp.where(lane8 == owner, row * 8 + local_ref[row, ch], by_owner)
            listed = jnp.where(lane8 == row * 8 + ch, owner, listed)
    r["codes0"][...] = jnp.where(row8 == 0, by_owner, listed)
    spread, pick, visible = masks()
    greeted()

    def z_has(d, k, i):
        return k < 4 or (k == 4 and (i < NB // 2) == (d == 0))

    def z_copy(d, k, i):
        sign = -1 if d == 0 else 1
        src, dst = sign * (k - 1), (4 if k == 4 else sign * k)
        return send(
            r[f"kv{src}"].at[i], r[f"kv{dst}"].at[i], "z", (d, k - 1, i), device(dz=1 if d == 0 else NZ - 1)
        )

    def z_event(k, i):
        for d in (0, 1):
            if z_has(d, k, i):
                z_copy(d, k, i).wait_recv()
                if z_has(d, k + 1, i):
                    z_copy(d, k + 1, i).start()
        if i == NB - 1:
            for dz in (-k, k) if k < 4 else (4,):
                pair(dz).start()

    def pair(dz):
        return send(r[f"kv{dz}"], r[f"other{dz}"], "p", dz + 3, device(flip=True))

    def y_query(j):
        return send(r["q0"], r[f"q{j}"], "y", j, device(dy=j))

    def y_codes(j):
        return send(r["codes0"], r[f"codes{j}"], "c", j, device(dy=j))

    def y_back(j, t):
        two = pl.ds(2 * t, 2)
        to = device(dy=NY - j)
        return (
            send(r["po"].at[j - 1, two], r["ro"].at[j - 1, two], "b", (j, t), to),
            send(r["pm"].at[j - 1, two], r["rm"].at[j - 1, two], "m", (j, t), to),
        )

    for i in range(NB):
        for d in (0, 1):
            z_copy(d, 1, i).start()
    for j in (2, 1, 3):
        y_codes(j).start()
        y_query(j).start()
    pair(0).start()

    def attend(q, k, v_t, causal=False):
        scores = dot(k, spread(q), NT) * (HEAD_SIZE**-0.5)
        if causal:
            scores = jnp.where(visible, scores, NEG)
        highest = jnp.max(scores, axis=0, keepdims=True)
        weights = jnp.exp(scores - highest)
        if causal:
            weights = jnp.where(visible, weights, 0.0)
        mass = jnp.sum(weights, axis=0, keepdims=True)
        return highest, mass, dot(v_t, spread(weights.astype(BF16)))

    def own(b, _=None):
        highest, mass, blended = attend(r["q0"][b], r["kv0"][b, 0], r["kv0"][b, 1], causal=True)
        r["own_m"][b, 0:1] = highest
        r["own_m"][b, 1:2] = mass
        r["own_o"][b] = blended

    lax.fori_loop(0, NB, own, None)
    for i in range(NB):
        z_event(1, i)
        if i == 2:
            for j in (1, 2, 3):
                y_codes(j).wait_recv()
            tables = [
                pltpu.make_async_copy(r[f"codes{j}"], r["codes_s"].at[j], r["s_codes"].at[j]) for j in range(4)
            ]
            for copy in tables:
                copy.start()
        if i == 4:
            for copy in tables:
                copy.wait()
    for j in (1, 2, 3):
        y_query(j).wait_recv()

    def group(dz, flip):
        if flip:
            pair(dz).wait_recv()
        ref = r[f"other{dz}" if flip else f"kv{dz}"]
        side = 1 - c if flip else c
        zz = lax.rem(z + dz + NZ, NZ)
        owner, slot = (zz * NY + y) * 2 + side, zz * 2 + side

        def items(_, __):
            for j in range(4):
                code = r["codes_s"][j, 0, owner]
                row, loc = lax.div(code, 8), lax.rem(code, 8)
                highest, mass, blended = attend(r[f"q{j}"][row], ref[loc, 0], ref[loc, 1])
                r["item_m"][j, slot, 0:1] = highest
                r["item_m"][j, slot, 1:2] = mass
                r["item_o"][j, slot] = blended

        lax.fori_loop(0, 1, items, None)

    groups = [(0, False), (0, True)]
    for k in (1, 2, 3):
        groups += [(-k, False), (k, False), (-k, True), (k, True)]
    groups += [(4, False), (4, True)]
    for i in range(NB):
        z_event(2, i)
        group(*groups[i])
    for i in range(NB):
        z_event(3, i)
        if i < 4:
            group(*groups[6 + i])
    for i in range(NB):
        z_event(4, i)
        if i % 2 == 0:
            group(*groups[10 + i // 2])
    for g in groups[13:]:
        group(*g)

    def merged(j, b, mine=False):
        parts = []
        for ch in range(CHOSEN):
            owner = r["codes_s"][j, 1, b * 8 + ch]
            ok = lax.rem(lax.div(owner, 2), NY) == y
            slot = lax.div(owner, 2 * NY) * 2 + lax.rem(owner, 2)
            here = jnp.broadcast_to(ok.astype(I32), (1, FEATS)) > 0
            parts.append((here, r["item_m"][j, slot, 0:1], r["item_m"][j, slot, 1:2], r["item_o"][j, slot]))
        if mine:
            yes = jnp.full((1, FEATS), True)
            parts.append((yes, r["own_m"][b, 0:1], r["own_m"][b, 1:2], r["own_o"][b]))
        tops = [jnp.where(here, m, NEG) for here, m, _, _ in parts]
        top = tops[0]
        for m in tops[1:]:
            top = jnp.maximum(top, m)
        mass = jnp.zeros((1, FEATS), F32)
        blended = jnp.zeros((BLOCK, FEATS), F32)
        for (here, _, l, o), m in zip(parts, tops):
            scale = jnp.where(here, jnp.exp(m - top), 0.0)
            mass = mass + scale * l
            blended = blended + scale * o
        return top, mass, blended

    def back(step, _):
        t, j = lax.div(step, 3), 1 + lax.rem(step, 3)
        for n in range(2):
            b = 2 * t + n
            top, mass, blended = merged(j, b)
            r["pm"][j - 1, b, 0:1] = top
            r["pm"][j - 1, b, 1:2] = mass
            r["po"][j - 1, b] = blended.astype(BF16)
        for copy in y_back(j, t):
            copy.start()

    lax.fori_loop(0, 3 * CH, back, None)

    def finish(t, _):
        held = [merged(0, 2 * t + n, mine=True) for n in range(2)]
        for j in (1, 2, 3):
            for copy in y_back(j, t):
                copy.wait_recv()
        for n in range(2):
            b = 2 * t + n
            parts = [held[n]] + [
                (r["rm"][j, b, 0:1], r["rm"][j, b, 1:2], r["ro"][j, b].astype(F32)) for j in range(3)
            ]
            top = parts[0][0]
            for m, _, _ in parts[1:]:
                top = jnp.maximum(top, m)
            mass = jnp.zeros((1, FEATS), F32)
            blended = jnp.zeros((BLOCK, FEATS), F32)
            for m, l, o in parts:
                scale = jnp.exp(m - top)
                mass = mass + scale * l
                blended = blended + scale * o
            attended = (blended / mass).astype(BF16)
            out_ref[pl.ds(b * BLOCK, BLOCK), :] = dot(pick, spread(attended), NT).astype(BF16)

    lax.fori_loop(0, CH, finish, None)

    for i in range(NB):
        for d in (0, 1):
            for k in (1, 2, 3, 4):
                if z_has(d, k, i):
                    z_copy(d, k, i).wait_send()
    for dz in range(-3, 5):
        pair(dz).wait_send()
    for j in (1, 2, 3):
        y_codes(j).wait_send()
        y_query(j).wait_send()
        for t in range(CH):
            for copy in y_back(j, t):
                copy.wait_send()


def close_scratch():
    shapes = {}
    for j in range(4):
        shapes[f"gain{j}"] = VMEM((8, FEATS), F32)
        if j:
            shapes[f"att{j}"] = VMEM((NB * BLOCK, FEATS), BF16)
    return shapes | sems(g=(4,), a=(4, CH))


def close(att_ref, wo0_ref, wo1_ref, wo2_ref, wo3_ref, gain_ref, out_ref, *refs):
    r = dict(zip(close_scratch(), refs))
    r["att0"] = att_ref
    wo = (wo0_ref, wo1_ref, wo2_ref, wo3_ref)
    send = sender(r)
    greeted = greet([device(dx=j) for j in (1, 2, 3)])
    r["gain0"][...] = jnp.broadcast_to(gain_ref[...], (8, FEATS))
    greeted()

    def x_gain(j):
        return send(r["gain0"], r[f"gain{j}"], "g", j, device(dx=j))

    def x_att(j, t):
        rows = rows_of(t, 2 * BLOCK)
        return send(r["att0"].at[rows], r[f"att{j}"].at[rows], "a", (j, t), device(dx=j))

    for j in (2, 1, 3):
        x_gain(j).start()
    for t in range(CH):
        for j in (2, 1, 3):
            x_att(j, t).start()
    for j in (1, 2, 3):
        x_gain(j).wait_recv()
    for t in range(CH):
        for j in (1, 2, 3):
            x_att(j, t).wait_recv()
        rows = rows_of(t, 2 * BLOCK)
        wide = [r[f"att{j}"][rows, :].astype(F32) for j in range(4)]
        squares = sum(jnp.sum(a * a, axis=1, keepdims=True) for a in wide)
        scale = lax.rsqrt(squares / (HEADS * HEAD_SIZE) + EPS)
        total = jnp.zeros((2 * BLOCK, PART), F32)
        for j in range(4):
            normed = (wide[j] * scale * r[f"gain{j}"][0:1, :]).astype(BF16)
            total = total + dot(normed, wo[j][...])
        out_ref[rows, :] = total.astype(BF16)

    for j in (1, 2, 3):
        x_gain(j).wait_send()
        for t in range(CH):
            x_att(j, t).wait_send()


def call(body, name, shapes, specs, outs, collective, flops, operands):
    vmem = pl.BlockSpec(memory_space=VMEM)
    return pl.pallas_call(
        body,
        out_shape=outs,
        in_specs=specs,
        out_specs=jax.tree.map(lambda _: vmem, outs),
        scratch_shapes=list(shapes.values()),
        compiler_params=pltpu.CompilerParams(
            collective_id=collective, has_side_effects=True, vmem_limit_bytes=24 * 2**20
        ),
        cost_estimate=pl.CostEstimate(flops=flops, bytes_accessed=2**20, transcendentals=0),
        name=name,
    )(*operands)


def on_device(tokens, query_weight, key_weight, value_weight, out_weight, norm_gain, chosen_owner, chosen_local):
    hbm = pl.BlockSpec(memory_space=pltpu.HBM)
    vmem = pl.BlockSpec(memory_space=VMEM)
    smem = pl.BlockSpec(memory_space=SMEM)
    x = lax.axis_index("tp")
    columns = [lax.dynamic_slice_in_dim(out_weight, lax.rem(x + j, NX) * PART, PART, 1) for j in range(NX)]
    shifted = columns[:1] + [
        lax.ppermute(columns[j], "tp", [(i, (i + j) % NX) for i in range(NX)]) for j in range(1, NX)
    ]
    keys_values = jax.ShapeDtypeStruct((NB, 2, BLOCK, FEATS), BF16)
    queries = jax.ShapeDtypeStruct((NB, BLOCK, FEATS), BF16)
    rows = NB * BLOCK
    kv, q = call(
        project, "project", project_scratch(), [hbm] * 4, (keys_values, queries), 0, 10**9,
        (tokens, query_weight, key_weight, value_weight),
    )
    att = call(
        attend_all, "attend", attend_scratch(), [vmem, vmem, smem, smem], jax.ShapeDtypeStruct((rows, FEATS), BF16),
        1, 10**10, (kv, q, chosen_owner, chosen_local),
    )
    return call(
        close, "close", close_scratch(), [vmem] * 6, jax.ShapeDtypeStruct((rows, PART), BF16), 2, 10**9,
        (att, *shifted, norm_gain.reshape(1, FEATS)),
    )


def solution(mesh):
    return jax.shard_map(
        on_device,
        mesh=mesh,
        in_specs=(
            P("kv", "tp"),
            P(None, "tp"),
            P(None, "tp"),
            P(None, "tp"),
            P("tp", None),
            P("tp"),
            P("kv", None),
            P("kv", None),
        ),
        out_specs=P("kv", "tp"),
        check_vma=False,
    )
```

```python
import jax
import jax.numpy as jnp
from jax import lax
from jax.experimental import pallas as pl
from jax.experimental.pallas import tpu as pltpu
from jax.sharding import PartitionSpec as P

MESH = pl.DeviceIdType.MESH
BF16, F32, I32 = jnp.bfloat16, jnp.float32, jnp.int32

HEADS = 8
HEAD_SIZE = 64
BLOCK = 64
CHOSEN = 8
NB = 6
FEATS = 128
PART = 256
NZ, NY, NX = 8, 4, 4
NEG = -1e30
EPS = 1e-06
CH = 3

NT = (((1,), (1,)), ((), ()))
NN = (((1,), (0,)), ((), ()))


def dot(a, b, dims=NN):
    return lax.dot_general(a, b, dims, preferred_element_type=F32)


def scratch():
    shapes = {}
    for j in range(4):
        shapes[f"tok{j}"] = pltpu.VMEM((NB * BLOCK, PART), BF16)
        shapes[f"wo{j}"] = pltpu.VMEM((FEATS, PART), BF16)
        shapes[f"gain{j}"] = pltpu.VMEM((8, FEATS), F32)
        shapes[f"q{j}"] = pltpu.VMEM((NB, BLOCK, FEATS), BF16)
        shapes[f"codes{j}"] = pltpu.VMEM((8, 128), I32)
        shapes[f"att{j}"] = pltpu.VMEM((NB * BLOCK, FEATS), BF16)
    for dz in range(-3, 5):
        shapes[f"kv{dz}"] = pltpu.VMEM((NB, 2, BLOCK, FEATS), BF16)
        shapes[f"other{dz}"] = pltpu.VMEM((NB, 2, BLOCK, FEATS), BF16)
    shapes["w"] = pltpu.VMEM((1024, 3 * FEATS), BF16)
    shapes["wo"] = pltpu.VMEM((FEATS, 1024), BF16)
    shapes["codes_s"] = pltpu.SMEM((4, 8, 128), I32)
    for name in ("p", "r"):
        shapes[name + "o"] = pltpu.VMEM((3, NB, BLOCK, FEATS), BF16)
        shapes[name + "m"] = pltpu.VMEM((3, NB, 8, FEATS), F32)
    shapes["item_o"] = pltpu.VMEM((4, 2 * NZ, BLOCK, FEATS), F32)
    shapes["item_m"] = pltpu.VMEM((4, 2 * NZ, 8, FEATS), F32)
    shapes["own_o"] = pltpu.VMEM((NB, BLOCK, FEATS), F32)
    shapes["own_m"] = pltpu.VMEM((NB, 8, FEATS), F32)
    dma = pltpu.SemaphoreType.DMA
    shapes["s_in"] = dma((5,))
    shapes["s_codes"] = dma((4,))
    for name, shape in dict(
        x=(3, NB), z=(2, 4, NB), p=(8,), y=(4, NB), c=(4,), w=(4,), g=(4,), b=(4, CH), m=(4, CH), a=(4, CH)
    ).items():
        shapes["s_" + name] = dma(shape)
        shapes["r_" + name] = dma(shape)
    return shapes


def kernel(tok_hbm, wq_hbm, wk_hbm, wv_hbm, wo_hbm, gain_ref, owner_ref, local_ref, out_ref, *refs):
    r = dict(zip(scratch().keys(), refs))
    kv, x = lax.axis_index("kv"), lax.axis_index("tp")
    c, y, z = lax.rem(kv, 2), lax.rem(lax.div(kv, 2), NY), lax.div(kv, 2 * NY)

    def at(dz=0, dy=0, dx=0, flip=False):
        zz, yy, xx = lax.rem(z + dz, NZ), lax.rem(y + dy, NY), lax.rem(x + dx, NX)
        return ((zz * NY + yy) * 2 + (1 - c if flip else c), xx)

    def send(src, dst, name, index, device):
        return pltpu.make_async_remote_copy(
            src_ref=src,
            dst_ref=dst,
            send_sem=r["s_" + name].at[index],
            recv_sem=r["r_" + name].at[index],
            device_id=device,
            device_id_type=MESH,
        )

    ins = [pltpu.make_async_copy(tok_hbm, r["tok0"], r["s_in"].at[0])]
    for n, ref in enumerate((wk_hbm, wv_hbm, wq_hbm)):
        ins.append(pltpu.make_async_copy(ref, r["w"].at[:, pl.ds(n * FEATS, FEATS)], r["s_in"].at[n + 1]))
    ins.append(pltpu.make_async_copy(wo_hbm, r["wo"], r["s_in"].at[4]))
    for copy in ins:
        copy.start()

    barrier = pltpu.get_barrier_semaphore()
    peers = [at(dx=j) for j in (1, 2, 3)] + [at(dy=j) for j in (1, 2, 3)] + [at(dz=1), at(dz=NZ - 1), at(flip=True)]
    for peer in peers:
        pl.semaphore_signal(barrier, inc=1, device_id=peer, device_id_type=MESH)

    lane8 = lax.broadcasted_iota(I32, (8, 128), 1)
    row8 = lax.broadcasted_iota(I32, (8, 128), 0)
    by_owner = jnp.zeros((8, 128), I32)
    listed = jnp.zeros((8, 128), I32)
    for row in range(NB):
        for ch in range(CHOSEN):
            owner = owner_ref[row, ch]
            by_owner = jnp.where(lane8 == owner, row * 8 + local_ref[row, ch], by_owner)
            listed = jnp.where(lane8 == row * 8 + ch, owner, listed)
    r["codes0"][...] = jnp.where(row8 == 0, by_owner, listed)
    r["gain0"][...] = jnp.broadcast_to(gain_ref[...], (8, FEATS))

    lane = lax.broadcasted_iota(I32, (BLOCK, FEATS), 1)
    sub = lax.broadcasted_iota(I32, (BLOCK, FEATS), 0)
    low = (lane < HEAD_SIZE).astype(F32).astype(BF16)
    high = (lane >= HEAD_SIZE).astype(F32).astype(BF16)
    pick = (lax.rem(lane, HEAD_SIZE) == sub).astype(F32).astype(BF16)

    def spread(a):
        return jnp.concatenate([a * low, a * high], axis=0)

    ins[0].wait()
    pl.semaphore_wait(barrier, len(peers))

    def rows_of(i, n=BLOCK):
        return pl.ds(i * n, n)

    def x_own(kind, i):
        return send(
            r["tok0"].at[rows_of(i)], r["tok1" if kind == 0 else "tok3"].at[rows_of(i)], "x", (kind, i), at(dx=1 if kind == 0 else 3)
        )

    def x_far(i):
        src, dx = ("tok1", 1) if i % 2 == 0 else ("tok3", 3)
        return send(r[src].at[rows_of(i)], r["tok2"].at[rows_of(i)], "x", (2, i), at(dx=dx))

    def z_has(d, k, i):
        return k < 4 or (k == 4 and (i < NB // 2) == (d == 0))

    def z_copy(d, k, i):
        sign = -1 if d == 0 else 1
        src, dst = sign * (k - 1), (4 if k == 4 else sign * k)
        return send(
            r[f"kv{src}"].at[i], r[f"kv{dst}"].at[i], "z", (d, k - 1, i), at(dz=1 if d == 0 else NZ - 1)
        )

    def z_event(k, i):
        for d in (0, 1):
            if z_has(d, k, i):
                z_copy(d, k, i).wait_recv()
                if z_has(d, k + 1, i):
                    z_copy(d, k + 1, i).start()
        if i == NB - 1:
            for dz in (-k, k) if k < 4 else (4,):
                pair(dz).start()

    def pair(dz):
        return send(r[f"kv{dz}"], r[f"other{dz}"], "p", dz + 3, at(flip=True))

    def y_query(j, i):
        return send(r["q0"].at[i], r[f"q{j}"].at[i], "y", (j, i), at(dy=j))

    def y_codes(j):
        return send(r["codes0"], r[f"codes{j}"], "c", j, at(dy=j))

    def x_wo(j):
        cols = pl.ds(pl.multiple_of(lax.rem(x + j, NX) * PART, PART), PART)
        return send(r["wo"].at[:, cols], r[f"wo{j}"], "w", j, at(dx=j))

    def x_gain(j):
        return send(r["gain0"], r[f"gain{j}"], "g", j, at(dx=j))

    def y_back(j, t):
        two = pl.ds(2 * t, 2)
        to = at(dy=NY - j)
        return (
            send(r["po"].at[j - 1, two], r["ro"].at[j - 1, two], "b", (j, t), to),
            send(r["pm"].at[j - 1, two], r["rm"].at[j - 1, two], "m", (j, t), to),
        )

    def x_att(j, t):
        rows = rows_of(t, 2 * BLOCK)
        return send(r["att0"].at[rows], r[f"att{j}"].at[rows], "a", (j, t), at(dx=j))

    sent = []

    def start(copy):
        copy.start()
        sent.append(copy)

    for i in (0, 1):
        x_own(0, i).start()
        x_own(1, i).start()
    for j in (2, 1, 3):
        y_codes(j).start()
    for copy in ins[1:4]:
        copy.wait()

    def project(i):
        x_far(i).wait_recv()

        def block(_, __):
            total = jnp.zeros((BLOCK, 3 * FEATS), F32)
            for j in range(4):
                part = pl.ds(pl.multiple_of(lax.rem(x + NX - j, NX) * PART, PART), PART)
                total = total + dot(r[f"tok{j}"][rows_of(i), :], r["w"][part, :])
            r["kv0"][i, 0] = total[:, :FEATS].astype(BF16)
            r["kv0"][i, 1] = dot(pick, spread(total[:, FEATS : 2 * FEATS].astype(BF16)), NT).astype(BF16)
            r["q0"][i] = total[:, 2 * FEATS :].astype(BF16)

        lax.fori_loop(0, 1, block, None)
        for d in (0, 1):
            z_copy(d, 1, i).start()
        for j in (2, 1, 3):
            y_query(j, i).start()

    for i in range(NB):
        x_own(0, i).wait_recv()
        x_own(1, i).wait_recv()
        x_far(i).start()
        if i + 2 < NB:
            x_own(0, i + 2).start()
            x_own(1, i + 2).start()
        if i >= 1:
            project(i - 1)
        if i >= 4:
            z_event(1, i - 4)
    project(NB - 1)
    pair(0).start()
    ins[4].wait()
    for j in (2, 1, 3):
        x_wo(j).start()
        x_gain(j).start()
    mine = pl.ds(pl.multiple_of(x * PART, PART), PART)
    r["wo0"][...] = r["wo"][:, mine]
    z_event(1, 2)

    def attend(q, k, v_t, causal=False):
        scores = dot(k, spread(q), NT) * (HEAD_SIZE**-0.5)
        if causal:
            visible = sub <= lax.rem(lane, HEAD_SIZE)
            scores = jnp.where(visible, scores, NEG)
        highest = jnp.max(scores, axis=0, keepdims=True)
        weights = jnp.exp(scores - highest)
        if causal:
            weights = jnp.where(visible, weights, 0.0)
        mass = jnp.sum(weights, axis=0, keepdims=True)
        return highest, mass, dot(v_t, spread(weights.astype(BF16)))

    def own(b, _=None):
        highest, mass, blended = attend(r["q0"][b], r["kv0"][b, 0], r["kv0"][b, 1], causal=True)
        r["own_m"][b, 0:1] = highest
        r["own_m"][b, 1:2] = mass
        r["own_o"][b] = blended

    lax.fori_loop(0, NB, own, None)
    z_event(1, 3)
    for j in (1, 2, 3):
        y_codes(j).wait_recv()
    tables = [pltpu.make_async_copy(r[f"codes{j}"], r["codes_s"].at[j], r["s_codes"].at[j]) for j in range(4)]
    for copy in tables:
        copy.start()
    z_event(1, 4)
    z_event(1, 5)
    for copy in tables:
        copy.wait()
    for i in range(NB):
        for j in (1, 2, 3):
            y_query(j, i).wait_recv()

    def group(dz, flip):
        if flip:
            pair(dz).wait_recv()
        ref = r[f"other{dz}" if flip else f"kv{dz}"]
        side = 1 - c if flip else c
        zz = lax.rem(z + dz + NZ, NZ)
        owner, slot = (zz * NY + y) * 2 + side, zz * 2 + side

        def items(_, __):
            for j in range(4):
                code = r["codes_s"][j, 0, owner]
                row, loc = lax.div(code, 8), lax.rem(code, 8)
                highest, mass, blended = attend(r[f"q{j}"][row], ref[loc, 0], ref[loc, 1])
                r["item_m"][j, slot, 0:1] = highest
                r["item_m"][j, slot, 1:2] = mass
                r["item_o"][j, slot] = blended

        lax.fori_loop(0, 1, items, None)

    groups = [(0, False), (0, True)]
    for k in (1, 2, 3):
        groups += [(-k, False), (k, False), (-k, True), (k, True)]
    groups += [(4, False), (4, True)]
    for i in range(NB):
        z_event(2, i)
        group(*groups[i])
    for i in range(NB):
        z_event(3, i)
        if i < 4:
            group(*groups[6 + i])
    for i in range(NB):
        z_event(4, i)
        if i % 2 == 0:
            group(*groups[10 + i // 2])
    for g in groups[13:]:
        group(*g)

    def merged(j, b, mine=False):
        parts = []
        for ch in range(CHOSEN):
            owner = r["codes_s"][j, 1, b * 8 + ch]
            ok = lax.rem(lax.div(owner, 2), NY) == y
            slot = lax.div(owner, 2 * NY) * 2 + lax.rem(owner, 2)
            here = jnp.broadcast_to(ok.astype(I32), (1, FEATS)) > 0
            parts.append((here, r["item_m"][j, slot, 0:1], r["item_m"][j, slot, 1:2], r["item_o"][j, slot]))
        if mine:
            yes = jnp.full((1, FEATS), True)
            parts.append((yes, r["own_m"][b, 0:1], r["own_m"][b, 1:2], r["own_o"][b]))
        tops = [jnp.where(here, m, NEG) for here, m, _, _ in parts]
        top = tops[0]
        for m in tops[1:]:
            top = jnp.maximum(top, m)
        mass = jnp.zeros((1, FEATS), F32)
        blended = jnp.zeros((BLOCK, FEATS), F32)
        for (here, _, l, o), m in zip(parts, tops):
            scale = jnp.where(here, jnp.exp(m - top), 0.0)
            mass = mass + scale * l
            blended = blended + scale * o
        return top, mass, blended

    def back(step, _):
        t, j = lax.div(step, 3), 1 + lax.rem(step, 3)
        for n in range(2):
            b = 2 * t + n
            top, mass, blended = merged(j, b)
            r["pm"][j - 1, b, 0:1] = top
            r["pm"][j - 1, b, 1:2] = mass
            r["po"][j - 1, b] = blended.astype(BF16)
        for copy in y_back(j, t):
            copy.start()

    lax.fori_loop(0, 3 * CH, back, None)

    def finish(t, _):
        held = [merged(0, 2 * t + n, mine=True) for n in range(2)]
        for j in (1, 2, 3):
            for copy in y_back(j, t):
                copy.wait_recv()
        for n in range(2):
            b = 2 * t + n
            parts = [held[n]] + [
                (r["rm"][j, b, 0:1], r["rm"][j, b, 1:2], r["ro"][j, b].astype(F32)) for j in range(3)
            ]
            top = parts[0][0]
            for m, _, _ in parts[1:]:
                top = jnp.maximum(top, m)
            mass = jnp.zeros((1, FEATS), F32)
            blended = jnp.zeros((BLOCK, FEATS), F32)
            for m, l, o in parts:
                scale = jnp.exp(m - top)
                mass = mass + scale * l
                blended = blended + scale * o
            attended = (blended / mass).astype(BF16)
            r["att0"][rows_of(b), :] = dot(pick, spread(attended), NT).astype(BF16)
        for j in (2, 1, 3):
            x_att(j, t).start()

    lax.fori_loop(0, CH, finish, None)

    for j in (1, 2, 3):
        x_wo(j).wait_recv()
        x_gain(j).wait_recv()
    def close(t, _):
        for j in (1, 2, 3):
            x_att(j, t).wait_recv()
        rows = rows_of(t, 2 * BLOCK)
        wide = [r[f"att{j}"][rows, :].astype(F32) for j in range(4)]
        squares = sum(jnp.sum(a * a, axis=1, keepdims=True) for a in wide)
        scale = lax.rsqrt(squares / (HEADS * HEAD_SIZE) + EPS)
        total = jnp.zeros((2 * BLOCK, PART), F32)
        for j in range(4):
            normed = (wide[j] * scale * r[f"gain{j}"][0:1, :]).astype(BF16)
            total = total + dot(normed, r[f"wo{j}"][...])
        out_ref[rows, :] = total.astype(BF16)

    lax.fori_loop(0, CH, close, None)

    for i in range(NB):
        x_own(0, i).wait_send()
        x_own(1, i).wait_send()
        x_far(i).wait_send()
        for j in (1, 2, 3):
            y_query(j, i).wait_send()
        for d in (0, 1):
            for k in (1, 2, 3, 4):
                if z_has(d, k, i):
                    z_copy(d, k, i).wait_send()
    for dz in range(-3, 5):
        pair(dz).wait_send()
    for j in (1, 2, 3):
        y_codes(j).wait_send()
        x_wo(j).wait_send()
        x_gain(j).wait_send()
        for t in range(CH):
            for copy in y_back(j, t):
                copy.wait_send()
            x_att(j, t).wait_send()


def on_device(tokens, query_weight, key_weight, value_weight, out_weight, norm_gain, chosen_owner, chosen_local):
    hbm = pl.BlockSpec(memory_space=pltpu.HBM)
    vmem = pl.BlockSpec(memory_space=pltpu.VMEM)
    smem = pl.BlockSpec(memory_space=pltpu.SMEM)
    return pl.pallas_call(
        kernel,
        out_shape=jax.ShapeDtypeStruct((NB * BLOCK, PART), BF16),
        in_specs=[hbm] * 5 + [vmem, smem, smem],
        out_specs=vmem,
        scratch_shapes=list(scratch().values()),
        compiler_params=pltpu.CompilerParams(collective_id=0, has_side_effects=True),
        name="attend",
    )(tokens, query_weight, key_weight, value_weight, out_weight, norm_gain.reshape(1, FEATS), chosen_owner, chosen_local)


def solution(mesh):
    return jax.shard_map(
        on_device,
        mesh=mesh,
        in_specs=(
            P("kv", "tp"),
            P(None, "tp"),
            P(None, "tp"),
            P(None, "tp"),
            P("tp", None),
            P("tp"),
            P("kv", None),
            P("kv", None),
        ),
        out_specs=P("kv", "tp"),
        check_vma=False,
    )
```

```python
import jax
import jax.numpy as jnp
from jax import lax
from jax.experimental import pallas as pl
from jax.experimental.pallas import tpu as pltpu
from jax.sharding import PartitionSpec as P

MESH = pl.DeviceIdType.MESH
BF16, F32, I32 = jnp.bfloat16, jnp.float32, jnp.int32

HEADS = 8
HEAD_SIZE = 64
BLOCK = 64
CHOSEN = 8
NB = 6
FEATS = 128
PART = 256
NZ, NY, NX = 8, 4, 4
NEG = -1e30
EPS = 1e-06
ASKED = 64
AHEAD = 3
DIRECT = (0, NB - 1)
CH = 3

NT = (((1,), (1,)), ((), ()))
NN = (((1,), (0,)), ((), ()))


def dot(a, b, dims=NN):
    return lax.dot_general(a, b, dims, preferred_element_type=F32)


def scratch():
    shapes = {}
    for j in range(4):
        shapes[f"tok{j}"] = pltpu.VMEM((NB * BLOCK, PART), BF16)
        shapes[f"wo{j}"] = pltpu.VMEM((FEATS, PART), BF16)
        shapes[f"gain{j}"] = pltpu.VMEM((8, FEATS), F32)
        shapes[f"q{j}"] = pltpu.VMEM((NB, BLOCK, FEATS), BF16)
        shapes[f"codes{j}"] = pltpu.VMEM((8, 128), I32)
        shapes[f"att{j}"] = pltpu.VMEM((NB * BLOCK, FEATS), BF16)
    for dz in range(-3, 5):
        shapes[f"kv{dz}"] = pltpu.VMEM((NB, 2, BLOCK, FEATS), BF16)
        shapes[f"other{dz}"] = pltpu.VMEM((NB, 2, BLOCK, FEATS), BF16)
    shapes["w"] = pltpu.VMEM((1024, 3 * FEATS), BF16)
    shapes["wo"] = pltpu.VMEM((FEATS, 1024), BF16)
    shapes["codes_s"] = pltpu.SMEM((4, 8, 128), I32)
    for name in ("p", "r"):
        shapes[name + "o"] = pltpu.VMEM((3, NB, BLOCK, FEATS), BF16)
        shapes[name + "m"] = pltpu.VMEM((3, CH, 8, FEATS), F32)
    for name in ("l", "e"):
        shapes[name + "o"] = pltpu.VMEM((3, 2, BLOCK, FEATS), BF16)
        shapes[name + "m"] = pltpu.VMEM((3, 8, FEATS), F32)
    shapes["item_o"] = pltpu.VMEM((4, 2 * NZ, BLOCK, FEATS), F32)
    shapes["item_m"] = pltpu.VMEM((4, 2 * NZ, 8, FEATS), F32)
    shapes["own_o"] = pltpu.VMEM((NB, BLOCK, FEATS), F32)
    shapes["own_m"] = pltpu.VMEM((NB, 8, FEATS), F32)
    dma = pltpu.SemaphoreType.DMA
    shapes["s_in"] = dma((5,))
    shapes["s_codes"] = dma((4,))
    for name, many, one in (
        ("x", (3, NB), (3,)),
        ("z", (2, 3, NB), (2, 3)),
        ("l", (NB,), (2,)),
        ("p", (8,), (8,)),
        ("y", (3,), (3,)),
        ("c", (3,), (3,)),
        ("w", (3,), (3,)),
        ("g", (3,), (3,)),
        ("b", (3,), (3,)),
        ("m", (3,), (3,)),
        ("e", (3,), (3,)),
        ("f", (3,), (3,)),
        ("a", (3, CH), (3,)),
    ):
        shapes["r_" + name] = dma(many)
        shapes["s_" + name] = dma(one)
    return shapes


def kernel(tok_hbm, wq_hbm, wk_hbm, wv_hbm, wo_hbm, gain_ref, owner_ref, local_ref, out_ref, *refs):
    r = dict(zip(scratch().keys(), refs))
    kv, x = lax.axis_index("kv"), lax.axis_index("tp")
    c, y, z = lax.rem(kv, 2), lax.rem(lax.div(kv, 2), NY), lax.div(kv, 2 * NY)

    def at(dz=0, dy=0, dx=0, flip=False):
        zz, yy, xx = lax.rem(z + dz, NZ), lax.rem(y + dy, NY), lax.rem(x + dx, NX)
        return ((zz * NY + yy) * 2 + (1 - c if flip else c), xx)

    def send(src, dst, name, group, index, device):
        return pltpu.make_async_remote_copy(
            src_ref=src,
            dst_ref=dst,
            send_sem=r["s_" + name].at[group],
            recv_sem=r["r_" + name].at[index],
            device_id=device,
            device_id_type=MESH,
        )

    ins = [pltpu.make_async_copy(tok_hbm, r["tok0"], r["s_in"].at[0])]
    for n, ref in enumerate((wk_hbm, wv_hbm, wq_hbm)):
        ins.append(pltpu.make_async_copy(ref, r["w"].at[:, pl.ds(n * FEATS, FEATS)], r["s_in"].at[n + 1]))
    ins.append(pltpu.make_async_copy(wo_hbm, r["wo"], r["s_in"].at[4]))
    for copy in ins:
        copy.start()

    barrier = pltpu.get_barrier_semaphore()
    peers = [at(dx=j) for j in (1, 2, 3)] + [at(dy=j) for j in (1, 2, 3)] + [at(dz=1), at(dz=NZ - 1), at(flip=True)]
    for peer in peers:
        pl.semaphore_signal(barrier, inc=1, device_id=peer, device_id_type=MESH)

    lane8 = lax.broadcasted_iota(I32, (8, 128), 1)
    row8 = lax.broadcasted_iota(I32, (8, 128), 0)
    by_owner = jnp.zeros((8, 128), I32)
    listed = jnp.zeros((8, 128), I32)
    for row in range(NB):
        for ch in range(CHOSEN):
            owner = owner_ref[row, ch]
            by_owner = jnp.where(lane8 == owner, ASKED + row * 8 + local_ref[row, ch], by_owner)
            listed = jnp.where(lane8 == row * 8 + ch, owner, listed)
    r["codes0"][...] = jnp.where(row8 == 0, by_owner, listed)
    r["gain0"][...] = jnp.broadcast_to(gain_ref[...], (8, FEATS))

    lane = lax.broadcasted_iota(I32, (BLOCK, FEATS), 1)
    sub = lax.broadcasted_iota(I32, (BLOCK, FEATS), 0)
    low = (lane < HEAD_SIZE).astype(F32).astype(BF16)
    high = (lane >= HEAD_SIZE).astype(F32).astype(BF16)
    pick = (lax.rem(lane, HEAD_SIZE) == sub).astype(F32).astype(BF16)

    def spread(a):
        return jnp.concatenate([a * low, a * high], axis=0)

    ins[0].wait()
    pl.semaphore_wait(barrier, len(peers))

    def rows_of(i, n=BLOCK):
        return pl.ds(i * n, n)

    def x_own(kind, i):
        return send(
            r["tok0"].at[rows_of(i)], r["tok1" if kind == 0 else "tok3"].at[rows_of(i)], "x", kind, (kind, i), at(dx=1 if kind == 0 else 3)
        )

    def x_far(i):
        if i in DIRECT:
            return send(r["tok0"].at[rows_of(i)], r["tok2"].at[rows_of(i)], "x", 2, (2, i), at(dx=2))
        src, dx = ("tok1", 1) if i % 2 == 0 else ("tok3", 3)
        return send(r[src].at[rows_of(i)], r["tok2"].at[rows_of(i)], "x", 2, (2, i), at(dx=dx))

    def z_has(d, k, i):
        return k < 4 or (k == 4 and (i < NB // 2) == (d == 0))

    def z_copy(d, k, i):
        sign = -1 if d == 0 else 1
        src, dst = sign * (k - 1), (4 if k == 4 else sign * k)
        to = at(dz=1 if d == 0 else NZ - 1)
        if k == 4:
            return send(r[f"kv{src}"].at[i], r["kv4"].at[i], "l", d, i, to)
        return send(r[f"kv{src}"].at[i], r[f"kv{dst}"].at[i], "z", (d, k - 1), (d, k - 1, i), to)

    def z_event(k, i):
        for d in (0, 1):
            if z_has(d, k, i):
                z_copy(d, k, i).wait_recv()
                if z_has(d, k + 1, i):
                    z_copy(d, k + 1, i).start()
        if i == NB - 1:
            for dz in (-k, k) if k < 4 else (4,):
                pair(dz).start()

    def pair(dz):
        return send(r[f"kv{dz}"], r[f"other{dz}"], "p", dz + 3, dz + 3, at(flip=True))

    def y_query(j, i):
        return send(r["q0"].at[i], r[f"q{j}"].at[i], "y", j - 1, j - 1, at(dy=j))

    def y_queries(j):
        return send(r["q0"], r[f"q{j}"], "y", j - 1, j - 1, at(dy=j))

    def y_codes(j):
        return send(r["codes0"], r[f"codes{j}"], "c", j - 1, j - 1, at(dy=j))

    def x_wo(j):
        cols = pl.ds(pl.multiple_of(lax.rem(x + j, NX) * PART, PART), PART)
        return send(r["wo"].at[:, cols], r[f"wo{j}"], "w", j - 1, j - 1, at(dx=j))

    def x_gain(j):
        return send(r["gain0"], r[f"gain{j}"], "g", j - 1, j - 1, at(dx=j))

    def y_back(j):
        to = at(dy=NY - j)
        return (
            send(r["po"].at[j - 1], r["ro"].at[j - 1], "b", j - 1, j - 1, to),
            send(r["pm"].at[j - 1], r["rm"].at[j - 1], "m", j - 1, j - 1, to),
        )

    def y_late(j):
        to = at(dy=NY - j)
        return (
            send(r["lo"].at[j - 1], r["eo"].at[j - 1], "e", j - 1, j - 1, to),
            send(r["lm"].at[j - 1], r["em"].at[j - 1], "f", j - 1, j - 1, to),
        )

    def x_att(j, t):
        rows = rows_of(t, 2 * BLOCK)
        return send(r["att0"].at[rows], r[f"att{j}"].at[rows], "a", j - 1, (j - 1, t), at(dx=j))

    sent = []

    def start(copy):
        copy.start()
        sent.append(copy)

    def x_start(i):
        x_own(0, i).start()
        x_own(1, i).start()
        if i in DIRECT:
            x_far(i).start()

    for i in range(AHEAD):
        x_start(i)
    for j in (2, 1, 3):
        y_codes(j).start()
    for copy in ins[1:4]:
        copy.wait()

    def project(i):
        x_far(i).wait_recv()

        def block(_, __):
            total = jnp.zeros((BLOCK, 3 * FEATS), F32)
            for j in range(4):
                part = pl.ds(pl.multiple_of(lax.rem(x + NX - j, NX) * PART, PART), PART)
                total = total + dot(r[f"tok{j}"][rows_of(i), :], r["w"][part, :])
            r["kv0"][i, 0] = total[:, :FEATS].astype(BF16)
            r["kv0"][i, 1] = dot(pick, spread(total[:, FEATS : 2 * FEATS].astype(BF16)), NT).astype(BF16)
            r["q0"][i] = dot(pick, spread(total[:, 2 * FEATS :].astype(BF16)), NT).astype(BF16)

        lax.fori_loop(0, 1, block, None)
        for d in (0, 1):
            z_copy(d, 1, i).start()
        for j in (2, 1, 3):
            y_query(j, i).start()

    for i in range(NB):
        x_own(0, i).wait_recv()
        x_own(1, i).wait_recv()
        if i not in DIRECT:
            x_far(i).start()
        if i + AHEAD < NB:
            x_start(i + AHEAD)
        if i >= 2:
            project(i - 2)
        if i >= 5:
            z_event(1, i - 5)
    project(NB - 2)
    z_event(1, 1)
    project(NB - 1)
    pair(0).start()
    ins[4].wait()
    for j in (2, 1, 3):
        x_wo(j).start()
        x_gain(j).start()
    mine = pl.ds(pl.multiple_of(x * PART, PART), PART)
    r["wo0"][...] = r["wo"][:, mine]
    z_event(1, 2)

    def attend(operands, causal=False):
        scores = [dot(k, spread(q)) * (HEAD_SIZE**-0.5) for q, k, _ in operands]
        if causal:
            visible = sub <= lax.rem(lane, HEAD_SIZE)
            scores = [jnp.where(visible, s, NEG) for s in scores]
        tops = [jnp.max(s, axis=0, keepdims=True) for s in scores]
        weights = [jnp.exp(s - top) for s, top in zip(scores, tops)]
        if causal:
            weights = [jnp.where(visible, w, 0.0) for w in weights]
        masses = [jnp.sum(w, axis=0, keepdims=True) for w in weights]
        blended = [dot(v, spread(w.astype(BF16))) for (_, _, v), w in zip(operands, weights)]
        return list(zip(tops, masses, blended))

    def own(half, _):
        found = attend(
            [(r["q0"][half * 3 + n], r["kv0"][half * 3 + n, 0], r["kv0"][half * 3 + n, 1]) for n in range(3)], causal=True
        )
        for n, (highest, mass, blended) in enumerate(found):
            b = half * 3 + n
            r["own_m"][b, 0:1] = highest
            r["own_m"][b, 1:2] = mass
            r["own_o"][b] = blended

    lax.fori_loop(0, 2, own, None)
    z_event(1, 3)
    for j in (1, 2, 3):
        y_codes(j).wait_recv()
    tables = [pltpu.make_async_copy(r[f"codes{j}"], r["codes_s"].at[j], r["s_codes"].at[j]) for j in range(4)]
    for copy in tables:
        copy.start()
    z_event(1, 4)
    z_event(1, 5)
    for copy in tables:
        copy.wait()
    for j in (1, 2, 3):
        y_queries(j).wait_recv()

    def group(*owners):
        for dz, flip in owners:
            if flip:
                pair(dz).wait_recv()

        def items(_, __):
            operands, places = [], []
            for dz, flip in owners:
                ref = r[f"other{dz}" if flip else f"kv{dz}"]
                side = 1 - c if flip else c
                zz = lax.rem(z + dz + NZ, NZ)
                owner, slot = (zz * NY + y) * 2 + side, zz * 2 + side
                for j in range(4):
                    code = r["codes_s"][j, 0, owner]
                    row, loc = lax.rem(lax.div(code, 8), 8), lax.rem(code, 8)
                    operands.append((r[f"q{j}"][row], ref[loc, 0], ref[loc, 1]))
                    places.append((j, slot, 1 if flip else 0))
            for (j, slot, n), (highest, mass, blended) in zip(places, attend(operands)):
                if owners[0][0] == 4 and j:
                    r["lm"][j - 1, n : n + 1] = highest
                    r["lm"][j - 1, 4 + n : 5 + n] = mass
                    r["lo"][j - 1, n] = blended.astype(BF16)
                else:
                    r["item_m"][j, slot, 0:1] = highest
                    r["item_m"][j, slot, 1:2] = mass
                    r["item_o"][j, slot] = blended

        lax.fori_loop(0, 1, items, None)

    def merged(j, b, mine=False):
        parts = []
        for ch in range(CHOSEN):
            owner = r["codes_s"][j, 1, b * 8 + ch]
            zz = lax.div(owner, 2 * NY)
            ok = jnp.logical_and(lax.rem(lax.div(owner, 2), NY) == y, zz != lax.rem(z + 4, NZ))
            slot = zz * 2 + lax.rem(owner, 2)
            here = jnp.broadcast_to(ok.astype(I32), (1, FEATS)) > 0
            parts.append((here, r["item_m"][j, slot, 0:1], r["item_m"][j, slot, 1:2], r["item_o"][j, slot]))
        if mine:
            yes = jnp.full((1, FEATS), True)
            parts.append((yes, r["own_m"][b, 0:1], r["own_m"][b, 1:2], r["own_o"][b]))
        tops = [jnp.where(here, m, NEG) for here, m, _, _ in parts]
        top = tops[0]
        for m in tops[1:]:
            top = jnp.maximum(top, m)
        mass = jnp.zeros((1, FEATS), F32)
        blended = jnp.zeros((BLOCK, FEATS), F32)
        for (here, _, l, o), m in zip(parts, tops):
            scale = jnp.where(here, jnp.exp(m - top), 0.0)
            mass = mass + scale * l
            blended = blended + scale * o
        return top, mass, blended

    def back(b, j):
        top, mass, blended = merged(j, b)
        t, n = lax.div(b, 2), lax.rem(b, 2)
        r["pm"][j - 1, t, pl.ds(n, 1)] = top
        r["pm"][j - 1, t, pl.ds(4 + n, 1)] = mass
        r["po"][j - 1, b] = blended.astype(BF16)
        return j

    def mine(b, _):
        top, mass, blended = merged(0, b, mine=True)
        r["own_m"][b, 2:3] = top
        r["own_m"][b, 3:4] = mass
        r["own_o"][b] = blended

    groups = [((0, False),), ((0, True),)]
    for k in (1, 2, 3):
        groups += [((-k, False), (k, False)), ((-k, True), (k, True))]
    groups += [((4, False),), ((4, True),)]
    for i in range(NB):
        z_event(2, i)
        if i < 4:
            group(*groups[i])
    for i in range(NB):
        z_event(3, i)
        if i in (1, 3):
            group(*groups[4 + i // 2])
    for i in range(NB):
        z_event(4, i)
        if i in (1, 3):
            group(*groups[6 + i // 2])
        if i == 3:
            for j in (2, 1, 3):
                lax.fori_loop(0, NB, back, j)
                for copy in y_back(j):
                    copy.start()
    lax.fori_loop(0, NB, mine, None)
    group(*groups[8])
    group(*groups[9])
    for j in (2, 1, 3):
        for copy in y_late(j):
            copy.start()
    for j in (1, 2, 3):
        for copy in y_back(j):
            copy.wait_recv()
    for j in (1, 2, 3):
        for copy in y_late(j):
            copy.wait_recv()

    def finish(t, _):
        for n in range(2):
            b = 2 * t + n
            parts = [(r["own_m"][b, 2:3], r["own_m"][b, 3:4], r["own_o"][b])]
            parts += [
                (r["rm"][j, t, n : n + 1], r["rm"][j, t, 4 + n : 5 + n], r["ro"][j, b].astype(F32)) for j in range(3)
            ]
            zz = lax.rem(z + 4, NZ)
            for j in range(4):
                for flip in (0, 1):
                    side = 1 - c if flip else c
                    owner = (zz * NY + lax.rem(y + j, NY)) * 2 + side
                    here = lax.div(r["codes_s"][0, 0, owner], 8) == ASKED // 8 + b
                    here = jnp.broadcast_to(here.astype(I32), (1, FEATS)) > 0
                    if j:
                        part = r["em"][j - 1, flip : flip + 1], r["em"][j - 1, 4 + flip : 5 + flip], r["eo"][j - 1, flip].astype(F32)
                    else:
                        slot = zz * 2 + side
                        part = r["item_m"][0, slot, 0:1], r["item_m"][0, slot, 1:2], r["item_o"][0, slot]
                    parts.append((jnp.where(here, part[0], NEG), jnp.where(here, part[1], 0.0), part[2], here))
            top = parts[0][0]
            for part in parts[1:]:
                top = jnp.maximum(top, part[0])
            mass = jnp.zeros((1, FEATS), F32)
            blended = jnp.zeros((BLOCK, FEATS), F32)
            for m, l, o, *here in parts:
                scale = jnp.exp(m - top)
                if here:
                    scale = jnp.where(here[0], scale, 0.0)
                mass = mass + scale * l
                blended = blended + scale * o
            attended = (blended / mass).astype(BF16)
            r["att0"][rows_of(b), :] = dot(pick, spread(attended), NT).astype(BF16)
        for j in (2, 1, 3):
            x_att(j, t).start()

    lax.fori_loop(0, CH, finish, None)
    for j in (1, 2, 3):
        x_wo(j).wait_recv()
        x_gain(j).wait_recv()

    def close(t, _):
        for j in (1, 2, 3):
            x_att(j, t).wait_recv()
        rows = rows_of(t, 2 * BLOCK)
        wide = [r[f"att{j}"][rows, :].astype(F32) for j in range(4)]
        squares = sum(jnp.sum(a * a, axis=1, keepdims=True) for a in wide)
        scale = lax.rsqrt(squares / (HEADS * HEAD_SIZE) + EPS)
        total = jnp.zeros((2 * BLOCK, PART), F32)
        for j in range(4):
            normed = (wide[j] * scale * r[f"gain{j}"][0:1, :]).astype(BF16)
            total = total + dot(normed, r[f"wo{j}"][...])
        out_ref[rows, :] = total.astype(BF16)

    lax.fori_loop(0, CH, close, None)

    def drain(ref, name, group):
        send(ref, ref, name, group, 0 if name in "lpycwgbmef" else (0, 0, 0) if name == "z" else (0, 0), at(flip=True)).wait_send()

    for kind in range(3):
        drain(r["tok0"], "x", kind)
    for d in (0, 1):
        for k in range(3):
            drain(r["kv0"], "z", (d, k))
        drain(r["kv0"].at[pl.ds(0, NB // 2)], "l", d)
    for dz in range(-3, 5):
        pair(dz).wait_send()
    for j in range(3):
        drain(r["q0"], "y", j)
        drain(r["codes0"], "c", j)
        drain(r["wo0"], "w", j)
        drain(r["gain0"], "g", j)
        drain(r["po"].at[j], "b", j)
        drain(r["pm"].at[j], "m", j)
        drain(r["lo"].at[j], "e", j)
        drain(r["lm"].at[j], "f", j)
        drain(r["att0"], "a", j)


def on_device(tokens, query_weight, key_weight, value_weight, out_weight, norm_gain, chosen_owner, chosen_local):
    hbm = pl.BlockSpec(memory_space=pltpu.HBM)
    vmem = pl.BlockSpec(memory_space=pltpu.VMEM)
    smem = pl.BlockSpec(memory_space=pltpu.SMEM)
    return pl.pallas_call(
        kernel,
        out_shape=jax.ShapeDtypeStruct((NB * BLOCK, PART), BF16),
        in_specs=[hbm] * 5 + [vmem, smem, smem],
        out_specs=vmem,
        scratch_shapes=list(scratch().values()),
        compiler_params=pltpu.CompilerParams(collective_id=0, has_side_effects=True),
        name="attend",
    )(tokens, query_weight, key_weight, value_weight, out_weight, norm_gain.reshape(1, FEATS), chosen_owner, chosen_local)


def solution(mesh):
    return jax.shard_map(
        on_device,
        mesh=mesh,
        in_specs=(
            P("kv", "tp"),
            P(None, "tp"),
            P(None, "tp"),
            P(None, "tp"),
            P("tp", None),
            P("tp"),
            P("kv", None),
            P("kv", None),
        ),
        out_specs=P("kv", "tp"),
        check_vma=False,
    )
```
